32 devices in a mesh: kv: 8 (over z, x), tp: 4 (over y, core).
Axes of the slice: x: 2, y: 2, z: 4, core: 2. Of those that a mesh axis runs over, the one named last changes fastest.
Arguments:
- tokens: bfloat16 [4096, 2048], P(('kv', 'tp')), may hold values from -6 to 6
- query_weight: bfloat16 [2048, 1024], P(None, 'tp'), may hold values from -0.125 to 0.125
- latent_weight: bfloat16 [2048, 256], replicated, may hold values from -0.125 to 0.125
- key_absorb: bfloat16 [8, 128, 256], P('tp'), may hold values from -0.5 to 0.5
- query_gain: bfloat16 [256], replicated, may hold values from 0.4 to 8
- latent_gain: bfloat16 [256], replicated, may hold values from 0.4 to 8
- value_absorb: bfloat16 [8, 256, 128], P('tp'), may hold values from -0.375 to 0.375
- head_gain: bfloat16 [8, 128], P('tp'), may hold values from 0.099609375 to 1.8984375
- out_weight: bfloat16 [1024, 2048], P('tp'), may hold values from -0.1875 to 0.1875
- chosen: int32 [64, 11], P('kv'), may hold values from 0 to 63, as said below
Outputs:
- mixed_out: bfloat16 [4096, 2048], P(('kv', 'tp'))
The draws below stay inside these ranges and needn't reach their ends.
Inputs may be any that keep to these rules, and one draw needn't show every extreme that they name: `chosen`: entry 0 of row b is b; a row's entries are distinct. Entries 1 to 3 lie in the same aligned run of 8 block numbers as b, the other 7 in other runs. For each aligned run of 8 rows and each other aligned run of 8 block numbers, those rows together name at most one block of that run. Entries above the row's own number may occur and contribute nothing.
All inputs are finite; a program needn't handle non-finite values.
Results may differ from the reference program's by a relative error of at most 0.014.
The reference program's roundings to bfloat16 on the way count: a program that leaves them out, or rounds other values in their place, can miss the bound.
Values may be sent and summed in bfloat16 or wider, within the bound.
No kernel may reach another device: no remote copies, remote signals or barrier semaphores. Data moves between devices by JAX's collectives and lax.ppermute only.
A program may use at most 64 MiB of HBM per device.

```python
import jax
import jax.numpy as jnp
from jax import lax

D = 2048
HEADS = 8
HEAD = 128
LATENT = 256
BLOCK = 64
TOKENS = 4096
NBLK = 64
SPAN_BLOCKS = 8
LOCAL_PICKS = 3
REMOTE = 7
NSEL = 11
HEAD_GROUP = 2
N_TP = 4


def gain_values(key, salt):
    base = jax.random.fold_in(key, salt)
    return jnp.clip(1.0 + 0.18 * jax.random.normal(base, (LATENT,), jnp.float32), 0.4, 1.6).astype(jnp.bfloat16)


def draw_query_gain(key, part):
    return gain_values(key, 11)


def draw_latent_gain(key, part):
    return gain_values(key, 23)


def draw_chosen(key, part):
    owners = NBLK // SPAN_BLOCKS
    first_key = jax.random.fold_in(key, 101)
    second_key = jax.random.fold_in(key, 202)
    third_key = jax.random.fold_in(key, 303)
    fourth_key = jax.random.fold_in(key, 404)
    block_pick = jax.random.randint(first_key, (owners, owners), 0, SPAN_BLOCKS)
    favored = (jax.random.randint(second_key, (owners,), 0, 4) == 0).astype(jnp.int32)
    row_ids = jnp.arange(NBLK, dtype=jnp.int32)
    device_of = row_ids // SPAN_BLOCKS
    local_pos = row_ids % SPAN_BLOCKS
    local_noise = jax.random.randint(third_key, (NBLK, SPAN_BLOCKS), 0, 1 << 20)
    local_range = jnp.arange(SPAN_BLOCKS, dtype=jnp.int32)
    local_score = local_noise * SPAN_BLOCKS + local_range[None, :]
    local_score = jnp.where(local_range[None, :] == local_pos[:, None], -1, local_score)
    _, local_pick = lax.top_k(local_score, LOCAL_PICKS)
    local_ids = device_of[:, None] * SPAN_BLOCKS + local_pick.astype(jnp.int32)
    owner_range = jnp.arange(owners, dtype=jnp.int32)
    remote_noise = jax.random.randint(fourth_key, (NBLK, owners), 0, 1 << 12)
    earlier = owner_range[None, :] < device_of[:, None]
    forced = (owner_range[None, :] == device_of[:, None] - 1) | (owner_range[None, :] == device_of[:, None] - owners // 2)
    level = jnp.where(forced, 3, jnp.where(earlier, 1, 0))
    level = jnp.where(owner_range[None, :] == device_of[:, None], -1, level)
    remote_score = (level * (1 << 13) + remote_noise + favored[None, :] * (1 << 11)) * owners + owner_range[None, :]
    _, remote_pick = lax.top_k(remote_score, REMOTE)
    remote_pick = remote_pick.astype(jnp.int32)
    remote_ids = remote_pick * SPAN_BLOCKS + block_pick[device_of[:, None], remote_pick]
    return jnp.concatenate([row_ids[:, None], local_ids, remote_ids], axis=1).astype(jnp.int32)


def block_scale(rng, dims, split, least, top_value):
    factor_of = 1.0
    for position, blocks in split:
        heights = jax.random.uniform(jax.random.fold_in(jax.random.fold_in(rng, 6), position), (blocks,), jnp.float32, least / len(split), top_value / len(split))
        factor_of = factor_of * jnp.repeat(jnp.exp(heights), dims[position] // blocks).reshape((-1,) + (1,) * (len(dims) - 1 - position))
    return factor_of


def scatter_about(stream_key, dims, width, reach, split=(), kind=jnp.bfloat16):
    values = jax.random.normal(stream_key, dims, jnp.float32) * width
    if len(split) > 0:
        values = block_scale(stream_key, dims, split, -0.22, 0.18) * values
    return jnp.clip(values, min=-reach, max=reach).astype(kind)


def setup_inputs(seed: int = 0) -> dict:
    keys = jax.random.split(jax.random.key(seed), 11)
    tokens = scatter_about(keys[0], (TOKENS, D), 1.0, 6.0, ((0, 32),))
    query_weight = scatter_about(keys[1], (D, HEADS * HEAD), D ** -0.5, 0.125, ((1, 4),))
    latent_weight = scatter_about(keys[2], (D, LATENT), D ** -0.5, 0.125)
    key_absorb = scatter_about(keys[3], (HEADS, HEAD, LATENT), HEAD ** -0.5, 0.5, ((0, 4),))
    query_gain = draw_query_gain(jax.random.fold_in(keys[10], 71), 0)
    latent_gain = draw_latent_gain(jax.random.fold_in(keys[10], 71), 0)
    value_absorb = scatter_about(keys[6], (HEADS, LATENT, HEAD), LATENT ** -0.5, 0.375, ((0, 4),))
    head_gain = jnp.clip(1.0 + 0.18 * jax.random.normal(keys[7], (HEADS, HEAD), jnp.float32), 0.099609375, 1.8984375).astype(jnp.bfloat16)
    out_weight = scatter_about(keys[8], (HEADS * HEAD, D), (HEADS * HEAD) ** -0.5, 0.1875, ((0, 4),))
    chosen = draw_chosen(jax.random.fold_in(keys[10], 71), 0)
    return {"tokens": tokens, "query_weight": query_weight, "latent_weight": latent_weight, "key_absorb": key_absorb, "query_gain": query_gain, "latent_gain": latent_gain, "value_absorb": value_absorb, "head_gain": head_gain, "out_weight": out_weight, "chosen": chosen}


epsilon = 1e-06

def normalize(values, gain):
    return values * lax.rsqrt(lax.optimization_barrier(jnp.mean(values * values, axis=-1, keepdims=True)) + epsilon) * gain

def reference(tokens, query_weight, latent_weight, key_absorb, query_gain, latent_gain, value_absorb, head_gain, out_weight, chosen):
    queries = jnp.dot(tokens, query_weight, preferred_element_type=jnp.float32).astype(jnp.bfloat16)
    latent = normalize(jnp.dot(tokens, latent_weight, preferred_element_type=jnp.float32), latent_gain.astype(jnp.float32)).astype(jnp.bfloat16)
    head_query = queries.reshape(TOKENS, HEADS, HEAD).astype(jnp.float32)
    absorbed = jnp.einsum('thd,hdc->thc', head_query, key_absorb.astype(jnp.float32))
    absorbed = normalize(absorbed, query_gain.astype(jnp.float32)).astype(jnp.bfloat16)
    key_blocks = latent.reshape(NBLK, BLOCK, LATENT)
    query_blocks = absorbed.reshape(NBLK, BLOCK, HEADS, LATENT)
    offsets = jnp.arange(BLOCK, dtype=jnp.int32)

    def attend(inputs):
        row_block, picked, block_index = inputs
        key_rows = key_blocks[picked].reshape(NSEL * BLOCK, LATENT).astype(jnp.float32)
        scores = jnp.einsum('qhc,kc->hqk', row_block.astype(jnp.float32), key_rows) * LATENT ** (-0.5)
        key_pos = (picked[:, None] * BLOCK + offsets[None, :]).reshape(NSEL * BLOCK)
        query_pos = block_index * BLOCK + offsets
        visible = key_pos[None, :] <= query_pos[:, None]
        scores = jnp.where(visible[None], scores, -jnp.inf)
        weights = lax.optimization_barrier(jax.nn.softmax(scores, axis=-1).astype(jnp.bfloat16)).astype(jnp.float32)
        return jnp.einsum('hqk,kc->qhc', weights, key_rows).astype(jnp.bfloat16)
    mixed = lax.map(attend, (query_blocks, chosen, jnp.arange(NBLK, dtype=jnp.int32)))
    mixed = mixed.reshape(TOKENS, HEADS, LATENT).astype(jnp.float32)
    values = jnp.einsum('thc,hcd->thd', mixed, value_absorb.astype(jnp.float32))
    head_out = normalize(values, head_gain.astype(jnp.float32)).astype(jnp.bfloat16).reshape(TOKENS, HEADS * HEAD)
    group_width = HEAD_GROUP * HEAD
    accumulated = jnp.zeros((TOKENS, D), jnp.float32)
    for group_index in range(N_TP):
        low = group_index * group_width
        partial_value = jnp.dot(head_out[:, low:low + group_width], out_weight[low:low + group_width], preferred_element_type=jnp.float32)
        accumulated = accumulated + lax.optimization_barrier(partial_value.astype(jnp.bfloat16)).astype(jnp.float32)
    return accumulated.astype(jnp.bfloat16)
```

```python
import functools

import jax
import jax.numpy as jnp
from jax import lax
from jax.experimental import pallas as pl
from jax.experimental.pallas import tpu as pltpu
from jax.sharding import PartitionSpec as P


epsilon = 1e-06
f32 = jnp.float32
bf16 = jnp.bfloat16
VMEM = pl.BlockSpec(memory_space=pltpu.VMEM)
SMEM = pl.BlockSpec(memory_space=pltpu.SMEM)


def rms(values, gain):
    return values * lax.rsqrt(jnp.mean(values * values, axis=-1, keepdims=True) + epsilon) * gain


def call(kernel, out_shape, in_specs, scratch=(), flops=0, moved=0, out_specs=None):
    many = isinstance(out_shape, (list, tuple))
    return pl.pallas_call(
        kernel,
        out_shape=out_shape,
        in_specs=in_specs,
        out_specs=out_specs or ([VMEM] * len(out_shape) if many else VMEM),
        scratch_shapes=list(scratch),
        cost_estimate=pl.CostEstimate(flops=flops, bytes_accessed=moved, transcendentals=0),
    )


def latent_kernel(tokens, weight, gain, out):
    product = jnp.dot(tokens[...], weight[...], preferred_element_type=f32)
    out[...] = rms(product, gain[...].astype(f32)).astype(bf16)


def pick_kernel(per_shard, asked, own, core, far, diag, table, outgoing):
    me = lax.axis_index("tp")
    rows = own.shape[0]
    block_len = rows // per_shard
    table[pl.ds(0, rows)] = own[...]
    table[pl.ds(rows, rows)] = core[...]
    table[pl.ds(2 * rows, rows)] = far[...]
    table[pl.ds(3 * rows, rows)] = diag[...]

    def one(index, carry):
        within = asked[index]
        slot = jnp.bitwise_xor(within // per_shard, me) * per_shard + within % per_shard
        source = pl.multiple_of(slot * block_len, block_len)
        target = pl.multiple_of(index * block_len, block_len)
        outgoing[pl.ds(target, block_len)] = table[pl.ds(source, block_len)]
        return carry

    lax.fori_loop(0, asked.shape[0], one, 0)


def absorb_kernel(pieces, *refs):
    tokens, (query_weight, key_absorb, gain, out) = refs[:pieces], refs[pieces:]
    heads, width, _ = key_absorb.shape
    scale = gain[...].astype(f32)
    for piece in range(pieces):
        queries = jnp.dot(tokens[piece][...], query_weight[...], preferred_element_type=f32).astype(bf16)
        for head in range(heads):
            part = queries[:, head * width : (head + 1) * width]
            out[piece, head] = rms(
                jnp.dot(part, key_absorb[head], preferred_element_type=f32), scale
            ).astype(bf16)


def attend_kernel(
    groups, chosen, absorbed, table, arrived, value_absorb, head_gain, out_weight, *rest
):
    outs, (store, keys, mixed) = rest[: len(groups)], rest[len(groups) :]
    me, span = lax.axis_index("tp"), lax.axis_index("kv")
    block_count, picks = chosen.shape
    span_rows = table.shape[0]
    block_len = span_rows // block_count
    _, heads, rows, latent_width = absorbed.shape
    per_shard = rows // block_len
    store[pl.ds(0, span_rows)] = table[...]
    store[pl.ds(span_rows, arrived.shape[0])] = arrived[...]
    lanes = heads * block_len
    key_row = lax.broadcasted_iota(jnp.int32, (block_len, lanes), 0)
    query_row = lax.broadcasted_iota(jnp.int32, (block_len, lanes), 1) % block_len
    causal = key_row <= query_row
    scale = latent_width ** (-0.5)
    for slot, group in enumerate(groups):
        for inner in range(per_shard):
            turn = (slot * per_shard + inner) % 2
            local = jnp.bitwise_xor(me, group) * per_shard + inner
            block = span * block_count + local
            seen = []
            for pick in range(picks):
                target = chosen[local, pick]
                owner, within = target // block_count, target % block_count
                near = jnp.bitwise_xor(within // per_shard, me) * per_shard + within % per_shard
                source = jnp.where(owner == span, near, block_count + owner) * block_len
                keys[turn, pl.ds(pick * block_len, block_len)] = store[
                    pl.ds(pl.multiple_of(source, block_len), block_len)
                ]
                seen.append(target < block)
            query = absorbed[slot, :, pl.ds(inner * block_len, block_len), :].reshape(
                lanes, latent_width
            )
            near_keys = keys[turn]
            scores = lax.dot_general(
                near_keys, query, (((1,), (1,)), ((), ())), preferred_element_type=f32
            ) * scale
            parts = []
            for pick in range(picks):
                part = scores[pick * block_len : (pick + 1) * block_len]
                if pick == 0:
                    part = jnp.where(causal, part, -jnp.inf)
                else:
                    part = part + jnp.where(seen[pick], 0.0, -jnp.inf).astype(f32)
                parts.append(part)
            scores = jnp.concatenate(parts, axis=0)
            top = jnp.max(scores, axis=0, keepdims=True)
            raised = jnp.exp(scores - top)
            total = jnp.sum(raised, axis=0, keepdims=True)
            weights = (raised * (1.0 / total)).astype(bf16)
            out = lax.dot_general(
                weights, near_keys, (((0,), (0,)), ((), ())), preferred_element_type=f32
            ).astype(bf16)
            first = slot * rows + inner * block_len
            for head in range(heads):
                mixed[head, pl.ds(first, block_len)] = out[
                    head * block_len : (head + 1) * block_len
                ]
    parts = []
    for head in range(heads):
        values = jnp.dot(mixed[head], value_absorb[head], preferred_element_type=f32)
        parts.append(rms(values, head_gain[pl.ds(head, 1)].astype(f32)).astype(bf16))
    head_out = jnp.concatenate(parts, axis=1)
    for slot in range(len(groups)):
        outs[slot][...] = jnp.dot(
            head_out[slot * rows : (slot + 1) * rows],
            out_weight[...],
            preferred_element_type=f32,
        ).astype(bf16)


def body(
    tokens,
    query_weight,
    latent_weight,
    key_absorb,
    query_gain,
    latent_gain,
    value_absorb,
    head_gain,
    out_weight,
    chosen,
):
    shards = lax.axis_size("tp")
    spans = lax.axis_size("kv")
    rows, model = tokens.shape
    heads, width, latent_width = key_absorb.shape
    block_count, picks = chosen.shape
    per_shard = block_count // shards
    block_len = rows // per_shard
    shape = jax.ShapeDtypeStruct

    def swap(array, step):
        return lax.ppermute(array, "tp", [(i, i ^ step) for i in range(shards)])

    owner_of = chosen // block_count
    within = chosen % block_count
    matches = owner_of[:, :, None] == jnp.arange(spans, dtype=jnp.int32)[None, None, :]
    wanted = jnp.max(jnp.where(matches, within[:, :, None], 0), axis=(0, 1))

    own = call(
        latent_kernel,
        shape((rows, latent_width), bf16),
        [VMEM] * 3,
        flops=2 * rows * model * latent_width,
    )(tokens, latent_weight, latent_gain)
    core = swap(own, 1)
    far = swap(own, 2)
    diag = swap(own, 3)
    asked = lax.all_to_all(wanted, "kv", split_axis=0, concat_axis=0, tiled=True)
    tokens_far = swap(tokens, 2)
    tokens_core = swap(tokens, 1)
    tokens_diag = swap(tokens_far, 1)
    table, outgoing = call(
        functools.partial(pick_kernel, per_shard),
        [
            shape((block_count * block_len, latent_width), bf16),
            shape((spans * block_len, latent_width), bf16),
        ],
        [SMEM] + [VMEM] * 4,
    )(asked, own, core, far, diag)
    arrived = lax.all_to_all(
        outgoing.reshape(spans, block_len, latent_width),
        "kv",
        split_axis=0,
        concat_axis=0,
        tiled=True,
    ).reshape(spans * block_len, latent_width)

    def absorb(pieces):
        return call(
            functools.partial(absorb_kernel, len(pieces)),
            shape((len(pieces), heads, rows, latent_width), bf16),
            [VMEM] * (len(pieces) + 3),
            flops=2 * len(pieces) * rows * model * heads * width,
        )(*pieces, query_weight, key_absorb, query_gain)

    near_queries = absorb([tokens, tokens_core])
    far_queries = absorb([tokens_far, tokens_diag])

    def attend(groups, queries):
        return call(
            functools.partial(attend_kernel, groups),
            [shape((rows, model), bf16)] * len(groups),
            [SMEM] + [VMEM] * 6,
            scratch=[
                pltpu.VMEM(((block_count + spans) * block_len, latent_width), bf16),
                pltpu.VMEM((2, picks * block_len, latent_width), bf16),
                pltpu.VMEM((heads, len(groups) * rows, latent_width), bf16),
            ],
            flops=8 * len(groups) * per_shard * heads * block_len * picks * block_len * latent_width,
        )(chosen, queries, table, arrived, value_absorb, head_gain, out_weight)

    far_sum, far_send = attend((2, 3), far_queries)
    far_got = swap(far_send, 1)
    far_total = (far_sum.astype(f32) + far_got.astype(f32)).astype(bf16)
    far_in = swap(far_total, 2)
    near_sum, near_send = attend((0, 1), near_queries)
    near_got = swap(near_send, 1)
    return (near_sum.astype(f32) + near_got.astype(f32) + far_in.astype(f32)).astype(bf16)


def solution(mesh):
    return jax.shard_map(
        body,
        mesh=mesh,
        in_specs=(
            P(("kv", "tp"), None),
            P(None, "tp"),
            P(),
            P("tp", None, None),
            P(),
            P(),
            P("tp", None, None),
            P("tp", None),
            P("tp", None),
            P("kv", None),
        ),
        out_specs=P(("kv", "tp"), None),
        check_vma=False,
    )
```

```python
import functools
import math

import jax
import jax.numpy as jnp
from jax import lax
from jax.experimental import pallas as pl
from jax.experimental.pallas import tpu as pltpu
from jax.sharding import PartitionSpec as P


epsilon = 1e-06
f32 = jnp.float32
bf16 = jnp.bfloat16
VMEM = pl.BlockSpec(memory_space=pltpu.VMEM)
SLACK = 2
LANES = 128
ABSORB = 8 << 20
FAR = 54 << 20
NEAR = 46 << 20
HBM = pl.BlockSpec(memory_space=pl.ANY)
SMEM = pl.BlockSpec(memory_space=pltpu.SMEM)


def split(value, count):
    if count & (count - 1) == 0:
        return value >> (count.bit_length() - 1), value & (count - 1)
    return value // count, value % count


def near_slot(within, me, per_shard):
    if per_shard & (per_shard - 1) == 0:
        return within ^ (me * per_shard)
    shard, inner = split(within, per_shard)
    return (shard ^ me) * per_shard + inner


def rms(values, gain):
    return values * lax.rsqrt(jnp.mean(values * values, axis=-1, keepdims=True) + epsilon) * gain


def call(kernel, out_shape, in_specs, scratch=(), flops=0, grant=None):
    many = isinstance(out_shape, (list, tuple))

    def run(*arrays):
        held = [array for array, spec in zip(arrays, in_specs) if spec is VMEM]
        held += list(out_shape) if many else [out_shape]
        held += [array for array in scratch if hasattr(array, "shape")]
        size = sum(math.prod(array.shape) * 2 for array in held)
        return pl.pallas_call(
            kernel,
            out_shape=out_shape,
            in_specs=in_specs,
            out_specs=[VMEM] * len(out_shape) if many else VMEM,
            scratch_shapes=list(scratch),
            compiler_params=pltpu.CompilerParams(vmem_limit_bytes=grant or size + (SLACK << 20)),
            cost_estimate=pl.CostEstimate(flops=flops, bytes_accessed=size, transcendentals=0),
        )(*arrays)

    return run


def pick_kernel(per_shard, asked, own, core, far, diag, outgoing, table):
    me = lax.axis_index("tp")
    rows = own.shape[0]
    block_len = rows // per_shard
    for index, part in enumerate((own, core, far, diag)):
        table[pl.ds(index * rows, rows)] = part[...]

    def one(index, carry):
        within = asked[index, 0, 0]
        slot = near_slot(within, me, per_shard)
        source = pl.multiple_of(slot * block_len, block_len)
        target = pl.multiple_of(index * block_len, block_len)
        outgoing[pl.ds(target, block_len)] = table[pl.ds(source, block_len)]
        return carry

    lax.fori_loop(0, asked.shape[0], one, 0)


def absorb_kernel(pieces, *refs):
    tokens, (query_weight, key_absorb, gain, out) = refs[:pieces], refs[pieces:]
    heads, width, _ = key_absorb.shape
    scale = gain[...].astype(f32)
    products = [
        jnp.dot(part[...], query_weight[...], preferred_element_type=f32) for part in tokens
    ]
    for piece in range(pieces):
        queries = products[piece].astype(bf16)
        for head in range(heads):
            part = queries[:, head * width : (head + 1) * width]
            out[piece, head] = rms(
                jnp.dot(part, key_absorb[head], preferred_element_type=f32), scale
            ).astype(bf16)


def attend_kernel(
    groups, chosen, absorbed, own, core, far, diag, arrived, value_absorb, head_gain, *rest
):
    out, store, keys, mixed = rest[-4:]
    me, span = lax.axis_index("tp"), lax.axis_index("kv")
    block_count, picks = chosen.shape
    _, heads, rows, latent_width = absorbed.shape
    span_rows = 4 * rows
    block_len = span_rows // block_count
    per_shard = rows // block_len
    width = keys.shape[1]
    for index, part in enumerate((own, core, far, diag)):
        store[pl.ds(index * rows, rows)] = part[...]
    store[pl.ds(span_rows, arrived.shape[0])] = arrived[...]
    lanes = heads * block_len
    query_row = lax.broadcasted_iota(jnp.int32, (lanes, LANES), 0) % block_len
    lane = lax.broadcasted_iota(jnp.int32, (lanes, LANES), 1)
    causal = lane <= query_row
    pick_of_lane = lax.broadcasted_iota(jnp.int32, (1, LANES), 1) // block_len
    per_tile = LANES // block_len
    scale = latent_width ** (-0.5) * math.log2(math.e)

    def gather(turn):
        slot, inner = turn // per_shard, turn % per_shard
        local = jnp.bitwise_xor(me, groups[slot]) * per_shard + inner
        block = span * block_count + local
        if width > picks * block_len:
            rest = width - picks * block_len
            keys[turn, pl.ds(picks * block_len, rest)] = jnp.zeros((rest, latent_width), bf16)
        biases = []
        for pick in range(picks):
            target = chosen[local, pick]
            owner, within = split(target, block_count)
            near = near_slot(within, me, per_shard)
            source = jnp.where(owner == span, near, block_count + owner) * block_len
            keys[turn, pl.ds(pick * block_len, block_len)] = store[
                pl.ds(pl.multiple_of(source, block_len), block_len)
            ]
            biases.append(jnp.where((target < block) | (pick == 0), 0.0, -jnp.inf).astype(f32))
        query = absorbed[groups[slot], :, pl.ds(inner * block_len, block_len), :].reshape(
            lanes, latent_width
        )
        scores = lax.dot_general(
            query, keys[turn], (((1,), (1,)), ((), ())), preferred_element_type=f32
        )
        return scores, biases

    def weigh(scores, biases):
        parts = []
        for tile in range(width // LANES):
            part = scores[:, tile * LANES : (tile + 1) * LANES]
            bias = jnp.full((1, LANES), -jnp.inf, f32)
            for inside in range(per_tile):
                pick = tile * per_tile + inside
                if pick < picks:
                    bias = jnp.where(pick_of_lane == inside, biases[pick], bias)
            part = part + bias
            if tile == 0:
                part = jnp.where(causal | (lane >= block_len), part, -jnp.inf)
            parts.append(part)
        top = parts[0]
        for part in parts[1:]:
            top = jnp.maximum(top, part)
        top = jnp.max(top, axis=1, keepdims=True)
        raised = [jnp.exp2((part - top) * scale) for part in parts]
        total = raised[0]
        for part in raised[1:]:
            total = total + part
        share = 1.0 / jnp.sum(total, axis=1, keepdims=True)
        return jnp.concatenate([(part * share).astype(bf16) for part in raised], axis=1)

    def mix(turn, weights):
        out = jnp.dot(weights, keys[turn], preferred_element_type=f32).astype(bf16)
        for head in range(heads):
            mixed[head, pl.ds(turn * block_len, block_len)] = out[
                head * block_len : (head + 1) * block_len
            ]

    turns = len(groups) * per_shard
    ahead = gather(0)
    for turn in range(turns):
        current = ahead
        if turn + 1 < turns:
            ahead = gather(turn + 1)
        mix(turn, weigh(*current))
    parts = []
    for head in range(heads):
        values = jnp.dot(mixed[head], value_absorb[head], preferred_element_type=f32)
        parts.append(rms(values, head_gain[pl.ds(head, 1)].astype(f32)).astype(bf16))
    head_out = jnp.concatenate(parts, axis=1)
    for weight in rest[:-4]:
        head_out = jnp.dot(head_out, weight[...], preferred_element_type=f32).astype(bf16)
    out[...] = head_out


def project_kernel(half, near, far, first, second, third, fourth, out):
    span = lax.axis_index("kv")
    parity = jnp.bitwise_and(jnp.bitwise_xor(span, span >> 1), 1)
    rows = out.shape[0]
    depth = 2 * first.shape[0]
    here = pl.ds(half * rows, rows)
    direct = jnp.concatenate([first[...], second[...]], axis=0)
    relayed = jnp.concatenate([third[...], fourth[...]], axis=0)
    at = pl.multiple_of(parity * depth, depth)
    other = pl.multiple_of((1 - parity) * depth, depth)
    partial = jnp.dot(far[here, pl.ds(at, depth)], direct, preferred_element_type=f32)
    partial += jnp.dot(far[here, pl.ds(other, depth)], relayed, preferred_element_type=f32)
    total = near[here].astype(f32) + partial.astype(bf16).astype(f32)
    out[...] = total.astype(out.dtype)


def body(
    tokens,
    query_weight,
    latent_weight,
    key_absorb,
    query_gain,
    latent_gain,
    value_absorb,
    head_gain,
    out_weight,
    chosen,
):
    shards = lax.axis_size("tp")
    spans = lax.axis_size("kv")
    rows, model = tokens.shape
    heads, width, latent_width = key_absorb.shape
    block_count, picks = chosen.shape
    per_shard = block_count // shards
    block_len = rows // per_shard
    padded = -(-picks * block_len // LANES) * LANES
    shape = jax.ShapeDtypeStruct

    def swap(array, step):
        return lax.ppermute(array, "tp", [(i, i ^ step) for i in range(shards)])

    owner_of = chosen // block_count
    within = chosen % block_count
    matches = owner_of[:, :, None] == jnp.arange(spans, dtype=jnp.int32)[None, None, :]
    wanted = jnp.max(jnp.where(matches, within[:, :, None], 0), axis=(0, 1))
    wanted = jnp.broadcast_to(wanted[:, None, None], (spans, 1, LANES))

    own = rms(
        jnp.dot(tokens, latent_weight, preferred_element_type=f32), latent_gain.astype(f32)
    ).astype(bf16)
    core = swap(own, 1)
    far = swap(own, 2)
    diag = swap(own, 3)
    asked = lax.all_to_all(wanted, "kv", split_axis=0, concat_axis=0, tiled=True)
    tokens_far = swap(tokens, 2)
    tokens_core = swap(tokens, 1)
    tokens_diag = swap(tokens_far, 1)
    parity = jnp.bitwise_and(lax.axis_index("kv") ^ (lax.axis_index("kv") >> 1), 1)
    quarter = out_weight.shape[0] // 4
    piece_a = lax.dynamic_slice(out_weight, (2 * quarter * parity, 0), (quarter, model))
    piece_b = lax.dynamic_slice(out_weight, (2 * quarter * parity + quarter, 0), (quarter, model))

    def relay(array, step):
        return lax.ppermute(array, "kv", [(i, i ^ step) for i in range(spans)])

    far_weights = [swap(piece_a, 2), swap(piece_b, 2)]
    far_weights.append(relay(far_weights[0], 1))
    far_weights.append(relay(far_weights[1], 2))
    outgoing = call(
        functools.partial(pick_kernel, per_shard),
        shape((spans * block_len, latent_width), bf16),
        [SMEM] + [VMEM] * 4,
        scratch=[pltpu.VMEM((block_count * block_len, latent_width), bf16)],
    )(asked, own, core, far, diag)
    arrived = lax.all_to_all(
        outgoing.reshape(spans, block_len, latent_width),
        "kv",
        split_axis=0,
        concat_axis=0,
        tiled=True,
    ).reshape(spans * block_len, latent_width)

    def absorb(pieces):
        return call(
            functools.partial(absorb_kernel, len(pieces)),
            shape((len(pieces), heads, rows, latent_width), bf16),
            [VMEM] * (len(pieces) + 3),
            flops=2 * len(pieces) * rows * model * heads * width,
            grant=ABSORB,
        )(*pieces, query_weight, key_absorb, query_gain)

    queries = absorb([tokens, tokens_core, tokens_far, tokens_diag])

    def attend(groups, grant=None, weight=()):
        return call(
            functools.partial(attend_kernel, groups),
            shape((len(groups) * rows, model if weight else heads * width), bf16),
            [SMEM] + [VMEM] * (8 + len(weight)),
            scratch=[
                pltpu.VMEM(((block_count + spans) * block_len, latent_width), bf16),
                pltpu.VMEM((len(groups) * per_shard, padded, latent_width), bf16),
                pltpu.VMEM((heads, len(groups) * rows, latent_width), bf16),
            ],
            flops=8 * len(groups) * per_shard * heads * block_len * picks * block_len * latent_width,
            grant=grant,
        )(chosen, queries, own, core, far, diag, arrived, value_absorb, head_gain, *weight)

    far_heads = attend((2, 3), FAR)
    far_heads = swap(far_heads, 2)
    near_part = attend((0, 1), NEAR, (out_weight,))

    def project(half, dtype):
        return call(
            functools.partial(project_kernel, half),
            shape((rows, model), dtype),
            [VMEM] * 6,
            flops=2 * rows * heads * width * model,
        )(near_part, far_heads, *far_weights)

    core_part = project(1, bf16)
    core_part = swap(core_part, 1)
    own_part = project(0, f32)
    return (own_part + core_part.astype(f32)).astype(bf16)


def solution(mesh):
    return jax.shard_map(
        body,
        mesh=mesh,
        in_specs=(
            P(("kv", "tp"), None),
            P(None, "tp"),
            P(),
            P("tp", None, None),
            P(),
            P(),
            P("tp", None, None),
            P("tp", None),
            P("tp", None),
            P("kv", None),
        ),
        out_specs=P(("kv", "tp"), None),
        check_vma=False,
    )
```

```python
import functools
import math

import jax
import jax.numpy as jnp
from jax import lax
from jax.experimental import pallas as pl
from jax.experimental.pallas import tpu as pltpu
from jax.sharding import PartitionSpec as P


epsilon = 1e-06
f32 = jnp.float32
bf16 = jnp.bfloat16
VMEM = pl.BlockSpec(memory_space=pltpu.VMEM)
SLACK = 2
LANES = 128
ABSORB = 60 << 20
FAR = 53 << 20
NEAR = 8 << 20
HBM = pl.BlockSpec(memory_space=pl.ANY)
SMEM = pl.BlockSpec(memory_space=pltpu.SMEM)


def split(value, count):
    if count & (count - 1) == 0:
        return value >> (count.bit_length() - 1), value & (count - 1)
    return value // count, value % count


def near_slot(within, me, per_shard):
    if per_shard & (per_shard - 1) == 0:
        return within ^ (me * per_shard)
    shard, inner = split(within, per_shard)
    return (shard ^ me) * per_shard + inner


def rms(values, gain):
    return values * lax.rsqrt(jnp.mean(values * values, axis=-1, keepdims=True) + epsilon) * gain


def call(kernel, out_shape, in_specs, scratch=(), flops=0, grant=None):
    many = isinstance(out_shape, (list, tuple))

    def run(*arrays):
        held = [array for array, spec in zip(arrays, in_specs) if spec is VMEM]
        held += list(out_shape) if many else [out_shape]
        held += [array for array in scratch if hasattr(array, "shape")]
        size = sum(math.prod(array.shape) * array.dtype.itemsize for array in held)
        return pl.pallas_call(
            kernel,
            out_shape=out_shape,
            in_specs=in_specs,
            out_specs=[VMEM] * len(out_shape) if many else VMEM,
            scratch_shapes=list(scratch),
            compiler_params=pltpu.CompilerParams(vmem_limit_bytes=max(grant or 0, size + (SLACK << 20))),
            cost_estimate=pl.CostEstimate(flops=flops, bytes_accessed=size, transcendentals=0),
        )(*arrays)

    return run


def wanted_kernel(block_count, chosen, wanted):
    owner, within = split(chosen[...], block_count)
    within = within.astype(f32)

    def one(index, carry):
        found = jnp.max(jnp.where(owner == index, within, 0.0))
        wanted[index] = jnp.full((1, LANES), found, f32).astype(jnp.int32)
        return carry

    lax.fori_loop(0, wanted.shape[0], one, 0, unroll=8)


def pick_kernel(per_shard, asked, own, core, far, diag, outgoing, table):
    me = lax.axis_index("tp")
    rows = own.shape[0]
    block_len = rows // per_shard
    for index, part in enumerate((own, core, far, diag)):
        table[pl.ds(index * rows, rows)] = part[...]

    def one(index, carry):
        within = asked[index, 0, 0]
        slot = near_slot(within, me, per_shard)
        source = pl.multiple_of(slot * block_len, block_len)
        target = pl.multiple_of(index * block_len, block_len)
        outgoing[pl.ds(target, block_len)] = table[pl.ds(source, block_len)]
        return carry

    lax.fori_loop(0, asked.shape[0], one, 0)


def absorb_kernel(pieces, *refs):
    tokens, (query_weight, key_absorb, gain, out) = refs[:pieces], refs[pieces:]
    heads, width, _ = key_absorb.shape
    scale = gain[...].astype(f32)
    products = [
        jnp.dot(part[...], query_weight[...], preferred_element_type=f32) for part in tokens
    ]
    for piece in range(pieces):
        queries = products[piece].astype(bf16)
        for head in range(heads):
            part = queries[:, head * width : (head + 1) * width]
            out[piece, head] = rms(
                jnp.dot(part, key_absorb[head], preferred_element_type=f32), scale
            ).astype(bf16)


def attend_kernel(
    groups, chosen, absorbed, own, core, far, diag, arrived, value_absorb, head_gain, *rest
):
    outs, (store, keys, mixed) = rest[:-3], rest[-3:]
    me, span = lax.axis_index("tp"), lax.axis_index("kv")
    block_count, picks = chosen.shape
    _, heads, rows, latent_width = absorbed.shape
    span_rows = 4 * rows
    block_len = span_rows // block_count
    per_shard = rows // block_len
    width = keys.shape[1]
    for index, part in enumerate((own, core, far, diag)):
        store[pl.ds(index * rows, rows)] = part[...]
    store[pl.ds(span_rows, arrived.shape[0])] = arrived[...]
    lanes = heads * block_len
    query_row = lax.broadcasted_iota(jnp.int32, (lanes, LANES), 0) % block_len
    lane = lax.broadcasted_iota(jnp.int32, (lanes, LANES), 1)
    causal = lane <= query_row
    pick_of_lane = lax.broadcasted_iota(jnp.int32, (1, LANES), 1) // block_len
    per_tile = LANES // block_len
    scale = latent_width ** (-0.5) * math.log2(math.e)

    def gather(turn):
        slot, inner = turn // per_shard, turn % per_shard
        local = jnp.bitwise_xor(me, groups[slot]) * per_shard + inner
        block = span * block_count + local
        if width > picks * block_len:
            rest = width - picks * block_len
            keys[turn, pl.ds(picks * block_len, rest)] = jnp.zeros((rest, latent_width), bf16)
        biases = []
        for pick in range(picks):
            target = chosen[local, pick]
            owner, within = split(target, block_count)
            near = near_slot(within, me, per_shard)
            source = jnp.where(owner == span, near, block_count + owner) * block_len
            keys[turn, pl.ds(pick * block_len, block_len)] = store[
                pl.ds(pl.multiple_of(source, block_len), block_len)
            ]
            biases.append(jnp.where((target < block) | (pick == 0), 0.0, -jnp.inf).astype(f32))
        query = absorbed[groups[slot], :, pl.ds(inner * block_len, block_len), :].reshape(
            lanes, latent_width
        )
        scores = lax.dot_general(
            query, keys[turn], (((1,), (1,)), ((), ())), preferred_element_type=f32
        )
        return scores, biases

    def weigh(scores, biases):
        parts = []
        for tile in range(width // LANES):
            part = scores[:, tile * LANES : (tile + 1) * LANES]
            bias = jnp.full((1, LANES), -jnp.inf, f32)
            for inside in range(per_tile):
                pick = tile * per_tile + inside
                if pick < picks:
                    bias = jnp.where(pick_of_lane == inside, biases[pick], bias)
            part = part + bias
            if tile == 0:
                part = jnp.where(causal | (lane >= block_len), part, -jnp.inf)
            parts.append(part)
        top = parts[0]
        for part in parts[1:]:
            top = jnp.maximum(top, part)
        top = jnp.max(top, axis=1, keepdims=True)
        raised = [jnp.exp2((part - top) * scale) for part in parts]
        total = raised[0]
        for part in raised[1:]:
            total = total + part
        share = 1.0 / jnp.sum(total, axis=1, keepdims=True)
        return jnp.concatenate([(part * share).astype(bf16) for part in raised], axis=1)

    def mix(turn, weights):
        out = jnp.dot(weights, keys[turn], preferred_element_type=f32).astype(bf16)
        for head in range(heads):
            mixed[head, pl.ds(turn * block_len, block_len)] = out[
                head * block_len : (head + 1) * block_len
            ]

    turns = len(groups) * per_shard
    ahead = gather(0)
    for turn in range(turns):
        current = ahead
        if turn + 1 < turns:
            ahead = gather(turn + 1)
        mix(turn, weigh(*current))
    parts = []
    for head in range(heads):
        values = jnp.dot(mixed[head], value_absorb[head], preferred_element_type=f32)
        parts.append(rms(values, head_gain[pl.ds(head, 1)].astype(f32)).astype(bf16))
    head_out = jnp.concatenate(parts, axis=1)
    if outs[-1].shape[0] == rows:
        for slot, out in enumerate(outs):
            out[...] = head_out[slot * rows : (slot + 1) * rows]
    else:
        weight, out = outs
        out[...] = jnp.dot(head_out, weight[...], preferred_element_type=f32).astype(bf16)


def project_kernel(half, near, far, first, second, third, fourth, out):
    span = lax.axis_index("kv")
    parity = jnp.bitwise_and(jnp.bitwise_xor(span, span >> 1), 1)
    rows = out.shape[0]
    depth = 2 * first.shape[0]
    here = pl.ds(half * rows, rows)
    direct = jnp.concatenate([first[...], second[...]], axis=0)
    relayed = jnp.concatenate([third[...], fourth[...]], axis=0)
    at = pl.multiple_of(parity * depth, depth)
    other = pl.multiple_of((1 - parity) * depth, depth)
    partial = jnp.dot(far[:, pl.ds(at, depth)], direct, preferred_element_type=f32)
    partial += jnp.dot(far[:, pl.ds(other, depth)], relayed, preferred_element_type=f32)
    total = near[here].astype(f32) + partial.astype(bf16).astype(f32)
    out[...] = total.astype(out.dtype)


def body(
    tokens,
    query_weight,
    latent_weight,
    key_absorb,
    query_gain,
    latent_gain,
    value_absorb,
    head_gain,
    out_weight,
    chosen,
):
    shards = lax.axis_size("tp")
    spans = lax.axis_size("kv")
    rows, model = tokens.shape
    heads, width, latent_width = key_absorb.shape
    block_count, picks = chosen.shape
    per_shard = block_count // shards
    block_len = rows // per_shard
    padded = -(-picks * block_len // LANES) * LANES
    shape = jax.ShapeDtypeStruct

    def swap(array, step):
        return lax.ppermute(array, "tp", [(i, i ^ step) for i in range(shards)])

    wanted = call(
        functools.partial(wanted_kernel, block_count), shape((spans, 1, LANES), jnp.int32), [VMEM]
    )(chosen)
    own = rms(
        jnp.dot(tokens, latent_weight, preferred_element_type=f32), latent_gain.astype(f32)
    ).astype(bf16)
    core = swap(own, 1)
    far = swap(own, 2)
    diag = swap(own, 3)
    asked = lax.all_to_all(wanted, "kv", split_axis=0, concat_axis=0, tiled=True)
    tokens_far = swap(tokens, 2)
    tokens_core = swap(tokens, 1)
    tokens_diag = swap(tokens_far, 1)
    parity = jnp.bitwise_and(lax.axis_index("kv") ^ (lax.axis_index("kv") >> 1), 1)
    quarter = out_weight.shape[0] // 4
    start = 2 * quarter * parity
    piece_a = lax.dynamic_slice(out_weight, (start, 0), (quarter, model))
    piece_b = lax.dynamic_slice(out_weight, (start + quarter, 0), (quarter, model))

    def relay(array, step):
        return lax.ppermute(array, "kv", [(i, i ^ step) for i in range(spans)])

    far_weights = [swap(piece_a, 2), swap(piece_b, 2)]
    far_weights.append(relay(far_weights[0], 1))
    far_weights.append(relay(far_weights[1], 2))
    outgoing = call(
        functools.partial(pick_kernel, per_shard),
        shape((spans * block_len, latent_width), bf16),
        [SMEM] + [VMEM] * 4,
        scratch=[pltpu.VMEM((block_count * block_len, latent_width), bf16)],
    )(asked, own, core, far, diag)
    arrived = lax.all_to_all(
        outgoing.reshape(spans, block_len, latent_width),
        "kv",
        split_axis=0,
        concat_axis=0,
        tiled=True,
    ).reshape(spans * block_len, latent_width)

    def absorb(pieces):
        return call(
            functools.partial(absorb_kernel, len(pieces)),
            shape((len(pieces), heads, rows, latent_width), bf16),
            [VMEM] * (len(pieces) + 3),
            flops=2 * len(pieces) * rows * model * heads * width,
            grant=ABSORB,
        )(*pieces, query_weight, key_absorb, query_gain)

    queries = absorb([tokens, tokens_core, tokens_far, tokens_diag])

    def attend(groups, grant=None, weight=()):
        return call(
            functools.partial(attend_kernel, groups),
            shape((len(groups) * rows, model), bf16)
            if weight
            else [shape((rows, heads * width), bf16)] * len(groups),
            [SMEM] + [VMEM] * (8 + len(weight)),
            scratch=[
                pltpu.VMEM(((block_count + spans) * block_len, latent_width), bf16),
                pltpu.VMEM((len(groups) * per_shard, padded, latent_width), bf16),
                pltpu.VMEM((heads, len(groups) * rows, latent_width), bf16),
            ],
            flops=8 * len(groups) * per_shard * heads * block_len * picks * block_len * latent_width,
            grant=grant,
        )(chosen, queries, own, core, far, diag, arrived, value_absorb, head_gain, *weight)

    far_own, far_core = attend((2, 3), FAR)
    far_core = swap(far_core, 2)
    far_own = swap(far_own, 2)
    near_part = attend((0, 1), NEAR, (out_weight,))

    def project(half, far_heads, dtype):
        return call(
            functools.partial(project_kernel, half),
            shape((rows, model), dtype),
            [VMEM] * 6,
            flops=2 * rows * heads * width * model,
        )(near_part, far_heads, *far_weights)

    core_part = project(1, far_core, bf16)
    core_part = swap(core_part, 1)
    own_part = project(0, far_own, f32)
    return (own_part + core_part.astype(f32)).astype(bf16)


def solution(mesh):
    return jax.shard_map(
        body,
        mesh=mesh,
        in_specs=(
            P(("kv", "tp"), None),
            P(None, "tp"),
            P(),
            P("tp", None, None),
            P(),
            P(),
            P("tp", None, None),
            P("tp", None),
            P("tp", None),
            P("kv", None),
        ),
        out_specs=P(("kv", "tp"), None),
        check_vma=False,
    )
```

```python
import functools
import math

import jax
import jax.numpy as jnp
from jax import lax
from jax.experimental import pallas as pl
from jax.experimental.pallas import tpu as pltpu
from jax.sharding import PartitionSpec as P


epsilon = 1e-06
f32 = jnp.float32
bf16 = jnp.bfloat16
VMEM = pl.BlockSpec(memory_space=pltpu.VMEM)
SLACK = 2
LANES = 128
ABSORB = 53 << 20
FAR = 8 << 20
NEAR = 8 << 20
HBM = pl.BlockSpec(memory_space=pl.ANY)
SMEM = pl.BlockSpec(memory_space=pltpu.SMEM)


def split(value, count):
    if count & (count - 1) == 0:
        return value >> (count.bit_length() - 1), value & (count - 1)
    return value // count, value % count


def near_slot(within, me, per_shard):
    if per_shard & (per_shard - 1) == 0:
        return within ^ (me * per_shard)
    shard, inner = split(within, per_shard)
    return (shard ^ me) * per_shard + inner


def rms(values, gain):
    return values * lax.rsqrt(jnp.mean(values * values, axis=-1, keepdims=True) + epsilon) * gain


def call(kernel, out_shape, in_specs, scratch=(), flops=0, grant=None):
    many = isinstance(out_shape, (list, tuple))

    def run(*arrays):
        held = [array for array, spec in zip(arrays, in_specs) if spec is VMEM]
        held += list(out_shape) if many else [out_shape]
        held += [array for array in scratch if hasattr(array, "shape")]
        size = sum(math.prod(array.shape) * array.dtype.itemsize for array in held)
        return pl.pallas_call(
            kernel,
            out_shape=out_shape,
            in_specs=in_specs,
            out_specs=[VMEM] * len(out_shape) if many else VMEM,
            scratch_shapes=list(scratch),
            compiler_params=pltpu.CompilerParams(vmem_limit_bytes=max(grant or 0, size + (SLACK << 20))),
            cost_estimate=pl.CostEstimate(flops=flops, bytes_accessed=size, transcendentals=0),
        )(*arrays)

    return run


def wanted_kernel(block_count, chosen, wanted):
    owner, within = split(chosen[...], block_count)
    within = within.astype(f32)

    def one(index, carry):
        found = jnp.max(jnp.where(owner == index, within, 0.0))
        wanted[index] = jnp.full((1, LANES), found, f32).astype(jnp.int32)
        return carry

    lax.fori_loop(0, wanted.shape[0], one, 0, unroll=8)


def pick_kernel(per_shard, asked, own, core, far, diag, outgoing, table):
    me = lax.axis_index("tp")
    rows = own.shape[0]
    block_len = rows // per_shard
    for index, part in enumerate((own, core, far, diag)):
        table[pl.ds(index * rows, rows)] = part[...]

    def one(index, carry):
        within = asked[index, 0, 0]
        slot = near_slot(within, me, per_shard)
        source = pl.multiple_of(slot * block_len, block_len)
        target = pl.multiple_of(index * block_len, block_len)
        outgoing[pl.ds(target, block_len)] = table[pl.ds(source, block_len)]
        return carry

    lax.fori_loop(0, asked.shape[0], one, 0)


def absorb_kernel(pieces, *refs):
    tokens, rest = refs[:pieces], refs[pieces:]
    query_weight, key_absorb, gain, chosen, head_gain, near, far, held, held_gain = rest
    held[...] = chosen[...]
    held_gain[...] = head_gain[...]
    heads, width, _ = key_absorb.shape
    scale = gain[...].astype(f32)
    products = [
        jnp.dot(part[...], query_weight[...], preferred_element_type=f32) for part in tokens
    ]
    for piece in range(pieces):
        queries = products[piece].astype(bf16)
        for head in range(heads):
            part = queries[:, head * width : (head + 1) * width]
            out, slot = (near, piece) if piece < pieces // 2 else (far, piece - pieces // 2)
            out[slot, head] = rms(
                jnp.dot(part, key_absorb[head], preferred_element_type=f32), scale
            ).astype(bf16)


def attend_kernel(
    groups, chosen, absorbed, own, core, far, diag, arrived, value_absorb, head_gain, *rest
):
    outs, (store, keys, mixed) = rest[:-3], rest[-3:]
    me, span = lax.axis_index("tp"), lax.axis_index("kv")
    block_count, picks = chosen.shape
    _, heads, rows, latent_width = absorbed.shape
    span_rows = 4 * rows
    block_len = span_rows // block_count
    per_shard = rows // block_len
    width = keys.shape[1]
    for index, part in enumerate((own, core, far, diag)):
        store[pl.ds(index * rows, rows)] = part[...]
    store[pl.ds(span_rows, arrived.shape[0])] = arrived[...]
    lanes = heads * block_len
    query_row = lax.broadcasted_iota(jnp.int32, (lanes, LANES), 0) % block_len
    lane = lax.broadcasted_iota(jnp.int32, (lanes, LANES), 1)
    causal = lane <= query_row
    pick_of_lane = lax.broadcasted_iota(jnp.int32, (1, LANES), 1) // block_len
    per_tile = LANES // block_len
    scale = latent_width ** (-0.5) * math.log2(math.e)

    def gather(turn):
        slot, inner = turn // per_shard, turn % per_shard
        local = jnp.bitwise_xor(me, groups[slot]) * per_shard + inner
        block = span * block_count + local
        if width > picks * block_len:
            rest = width - picks * block_len
            keys[turn, pl.ds(picks * block_len, rest)] = jnp.zeros((rest, latent_width), bf16)
        biases = []
        for pick in range(picks):
            target = chosen[local, pick]
            owner, within = split(target, block_count)
            near = near_slot(within, me, per_shard)
            source = jnp.where(owner == span, near, block_count + owner) * block_len
            keys[turn, pl.ds(pick * block_len, block_len)] = store[
                pl.ds(pl.multiple_of(source, block_len), block_len)
            ]
            biases.append(jnp.where((target < block) | (pick == 0), 0.0, -jnp.inf).astype(f32))
        query = absorbed[slot, :, pl.ds(inner * block_len, block_len), :].reshape(
            lanes, latent_width
        )
        scores = lax.dot_general(
            query, keys[turn], (((1,), (1,)), ((), ())), preferred_element_type=f32
        )
        return scores, biases

    def weigh(scores, biases):
        parts = []
        for tile in range(width // LANES):
            part = scores[:, tile * LANES : (tile + 1) * LANES]
            bias = jnp.full((1, LANES), -jnp.inf, f32)
            for inside in range(per_tile):
                pick = tile * per_tile + inside
                if pick < picks:
                    bias = jnp.where(pick_of_lane == inside, biases[pick], bias)
            part = part + bias
            if tile == 0:
                part = jnp.where(causal | (lane >= block_len), part, -jnp.inf)
            parts.append(part)
        top = parts[0]
        for part in parts[1:]:
            top = jnp.maximum(top, part)
        top = jnp.max(top, axis=1, keepdims=True)
        raised = [jnp.exp2((part - top) * scale) for part in parts]
        total = raised[0]
        for part in raised[1:]:
            total = total + part
        share = 1.0 / jnp.sum(total, axis=1, keepdims=True)
        return jnp.concatenate([(part * share).astype(bf16) for part in raised], axis=1)

    def mix(turn, weights):
        out = jnp.dot(weights, keys[turn], preferred_element_type=f32).astype(bf16)
        for head in range(heads):
            mixed[head, pl.ds(turn * block_len, block_len)] = out[
                head * block_len : (head + 1) * block_len
            ]

    turns = len(groups) * per_shard
    ahead = gather(0)
    for turn in range(turns):
        current = ahead
        if turn + 1 < turns:
            ahead = gather(turn + 1)
        mix(turn, weigh(*current))
    parts = []
    for head in range(heads):
        values = jnp.dot(mixed[head], value_absorb[head], preferred_element_type=f32)
        parts.append(rms(values, head_gain[pl.ds(head, 1)].astype(f32)).astype(bf16))
    head_out = jnp.concatenate(parts, axis=1)
    if outs[-1].shape[0] == rows:
        for slot, out in enumerate(outs):
            out[...] = head_out[slot * rows : (slot + 1) * rows]
    else:
        weight, out = outs
        out[...] = jnp.dot(head_out, weight[...], preferred_element_type=f32).astype(bf16)


def project_kernel(half, near, far, first, second, third, fourth, out):
    span = lax.axis_index("kv")
    parity = jnp.bitwise_and(jnp.bitwise_xor(span, span >> 1), 1)
    rows = out.shape[0]
    depth = 2 * first.shape[0]
    here = pl.ds(half * rows, rows)
    direct = jnp.concatenate([first[...], second[...]], axis=0)
    relayed = jnp.concatenate([third[...], fourth[...]], axis=0)
    at = pl.multiple_of(parity * depth, depth)
    other = pl.multiple_of((1 - parity) * depth, depth)
    partial = jnp.dot(far[:, pl.ds(at, depth)], direct, preferred_element_type=f32)
    partial += jnp.dot(far[:, pl.ds(other, depth)], relayed, preferred_element_type=f32)
    total = near[here].astype(f32) + partial.astype(bf16).astype(f32)
    out[...] = total.astype(out.dtype)


def body(
    tokens,
    query_weight,
    latent_weight,
    key_absorb,
    query_gain,
    latent_gain,
    value_absorb,
    head_gain,
    out_weight,
    chosen,
):
    shards = lax.axis_size("tp")
    spans = lax.axis_size("kv")
    rows, model = tokens.shape
    heads, width, latent_width = key_absorb.shape
    block_count, picks = chosen.shape
    per_shard = block_count // shards
    block_len = rows // per_shard
    padded = -(-picks * block_len // LANES) * LANES
    shape = jax.ShapeDtypeStruct

    def swap(array, step):
        return lax.ppermute(array, "tp", [(i, i ^ step) for i in range(shards)])

    wanted = call(
        functools.partial(wanted_kernel, block_count), shape((spans, 1, LANES), jnp.int32), [VMEM]
    )(chosen)
    own = rms(
        jnp.dot(tokens, latent_weight, preferred_element_type=f32), latent_gain.astype(f32)
    ).astype(bf16)
    core = swap(own, 1)
    far = swap(own, 2)
    diag = swap(own, 3)
    asked = lax.all_to_all(wanted, "kv", split_axis=0, concat_axis=0, tiled=True)
    tokens_far = swap(tokens, 2)
    tokens_core = swap(tokens, 1)
    tokens_diag = swap(tokens_far, 1)
    parity = jnp.bitwise_and(lax.axis_index("kv") ^ (lax.axis_index("kv") >> 1), 1)
    quarter = out_weight.shape[0] // 4
    start = 2 * quarter * parity
    piece_a = lax.dynamic_slice(out_weight, (start, 0), (quarter, model))
    piece_b = lax.dynamic_slice(out_weight, (start + quarter, 0), (quarter, model))

    def relay(array, step):
        return lax.ppermute(array, "kv", [(i, i ^ step) for i in range(spans)])

    far_weights = [swap(piece_a, 2), swap(piece_b, 2)]
    far_weights.append(relay(far_weights[0], 1))
    far_weights.append(relay(far_weights[1], 2))
    outgoing = call(
        functools.partial(pick_kernel, per_shard),
        shape((spans * block_len, latent_width), bf16),
        [SMEM] + [VMEM] * 4,
        scratch=[pltpu.VMEM((block_count * block_len, latent_width), bf16)],
    )(asked, own, core, far, diag)
    arrived = lax.all_to_all(
        outgoing.reshape(spans, block_len, latent_width),
        "kv",
        split_axis=0,
        concat_axis=0,
        tiled=True,
    ).reshape(spans * block_len, latent_width)

    def absorb(pieces):
        return call(
            functools.partial(absorb_kernel, len(pieces)),
            [shape((len(pieces) // 2, heads, rows, latent_width), bf16)] * 2
            + [shape(chosen.shape, chosen.dtype), shape(head_gain.shape, bf16)],
            [VMEM] * (len(pieces) + 5),
            flops=2 * len(pieces) * rows * model * heads * width,
            grant=ABSORB,
        )(*pieces, query_weight, key_absorb, query_gain, chosen, head_gain)

    near_queries, far_queries, held, held_gain = absorb([tokens, tokens_core, tokens_far, tokens_diag])

    def attend(groups, queries, grant=None, weight=()):
        return call(
            functools.partial(attend_kernel, groups),
            shape((len(groups) * rows, model), bf16)
            if weight
            else [shape((rows, heads * width), bf16)] * len(groups),
            [SMEM] + [VMEM] * (8 + len(weight)),
            scratch=[
                pltpu.VMEM(((block_count + spans) * block_len, latent_width), bf16),
                pltpu.VMEM((len(groups) * per_shard, padded, latent_width), bf16),
                pltpu.VMEM((heads, len(groups) * rows, latent_width), bf16),
            ],
            flops=8 * len(groups) * per_shard * heads * block_len * picks * block_len * latent_width,
            grant=grant,
        )(held, queries, own, core, far, diag, arrived, value_absorb, held_gain, *weight)

    far_own, far_core = attend((2, 3), far_queries, FAR)
    far_core = swap(far_core, 2)
    far_own = swap(far_own, 2)
    near_part = attend((0, 1), near_queries, NEAR, (out_weight,))

    def project(half, far_heads, dtype):
        return call(
            functools.partial(project_kernel, half),
            shape((rows, model), dtype),
            [VMEM] * 6,
            flops=2 * rows * heads * width * model,
        )(near_part, far_heads, *far_weights)

    core_part = project(1, far_core, bf16)
    core_part = swap(core_part, 1)
    own_part = project(0, far_own, f32)
    return (own_part + core_part.astype(f32)).astype(bf16)


def solution(mesh):
    return jax.shard_map(
        body,
        mesh=mesh,
        in_specs=(
            P(("kv", "tp"), None),
            P(None, "tp"),
            P(),
            P("tp", None, None),
            P(),
            P(),
            P("tp", None, None),
            P("tp", None),
            P("tp", None),
            P("kv", None),
        ),
        out_specs=P(("kv", "tp"), None),
        check_vma=False,
    )
```

```python
import functools
import math

import jax
import jax.numpy as jnp
from jax import lax
from jax.experimental import pallas as pl
from jax.experimental.pallas import tpu as pltpu
from jax.sharding import PartitionSpec as P


epsilon = 1e-06
f32 = jnp.float32
bf16 = jnp.bfloat16
VMEM = pl.BlockSpec(memory_space=pltpu.VMEM)
SLACK = 2
LANES = 128
ABSORB = 53 << 20
FAR = 8 << 20
NEAR = 8 << 20
HBM = pl.BlockSpec(memory_space=pl.ANY)
SMEM = pl.BlockSpec(memory_space=pltpu.SMEM)


def split(value, count):
    if count & (count - 1) == 0:
        return value >> (count.bit_length() - 1), value & (count - 1)
    return value // count, value % count


def near_slot(within, me, per_shard):
    if per_shard & (per_shard - 1) == 0:
        return within ^ (me * per_shard)
    shard, inner = split(within, per_shard)
    return (shard ^ me) * per_shard + inner


def rms(values, gain):
    return values * lax.rsqrt(jnp.mean(values * values, axis=-1, keepdims=True) + epsilon) * gain


def call(kernel, out_shape, in_specs, scratch=(), flops=0, grant=None):
    many = isinstance(out_shape, (list, tuple))

    def run(*arrays):
        held = [array for array, spec in zip(arrays, in_specs) if spec is VMEM]
        held += list(out_shape) if many else [out_shape]
        held += [array for array in scratch if hasattr(array, "shape")]
        size = sum(math.prod(array.shape) * array.dtype.itemsize for array in held)
        return pl.pallas_call(
            kernel,
            out_shape=out_shape,
            in_specs=in_specs,
            out_specs=[VMEM] * len(out_shape) if many else VMEM,
            scratch_shapes=list(scratch),
            compiler_params=pltpu.CompilerParams(vmem_limit_bytes=max(grant or 0, size + (SLACK << 20))),
            cost_estimate=pl.CostEstimate(flops=flops, bytes_accessed=size, transcendentals=0),
        )(*arrays)

    return run


def wanted_kernel(block_count, chosen, wanted):
    owner, within = split(chosen[...], block_count)
    within = within.astype(f32)

    def one(index, carry):
        found = jnp.max(jnp.where(owner == index, within, 0.0))
        wanted[index] = jnp.full((1, LANES), found, f32).astype(jnp.int32)
        return carry

    lax.fori_loop(0, wanted.shape[0], one, 0, unroll=8)


def pick_kernel(per_shard, asked, own, core, far, diag, outgoing, table):
    me = lax.axis_index("tp")
    rows = own.shape[0]
    block_len = rows // per_shard
    for index, part in enumerate((own, core, far, diag)):
        table[pl.ds(index * rows, rows)] = part[...]

    def one(index, carry):
        within = asked[index, 0, 0]
        slot = near_slot(within, me, per_shard)
        source = pl.multiple_of(slot * block_len, block_len)
        target = pl.multiple_of(index * block_len, block_len)
        outgoing[pl.ds(target, block_len)] = table[pl.ds(source, block_len)]
        return carry

    lax.fori_loop(0, asked.shape[0], one, 0)


def absorb_kernel(pieces, *refs):
    tokens, rest = refs[:pieces], refs[pieces:]
    query_weight, key_absorb, gain, chosen, head_gain, near, far, held, held_gain = rest
    held[...] = chosen[...]
    held_gain[...] = head_gain[...]
    heads, width, _ = key_absorb.shape
    scale = gain[...].astype(f32)
    products = [
        jnp.dot(part[...], query_weight[...], preferred_element_type=f32) for part in tokens
    ]
    for piece in range(pieces):
        queries = products[piece].astype(bf16)
        for head in range(heads):
            part = queries[:, head * width : (head + 1) * width]
            out, slot = (near, piece) if piece < pieces // 2 else (far, piece - pieces // 2)
            out[slot, head] = rms(
                jnp.dot(part, key_absorb[head], preferred_element_type=f32), scale
            ).astype(bf16)


def attend_kernel(
    groups, chosen, absorbed, own, core, far, diag, arrived, value_absorb, head_gain, *rest
):
    outs, (store, keys, mixed) = rest[:-3], rest[-3:]
    me, span = lax.axis_index("tp"), lax.axis_index("kv")
    block_count, picks = chosen.shape
    _, heads, rows, latent_width = absorbed.shape
    span_rows = 4 * rows
    block_len = span_rows // block_count
    per_shard = rows // block_len
    width = keys.shape[1]
    for index, part in enumerate((own, core, far, diag)):
        store[pl.ds(index * rows, rows)] = part[...]
    store[pl.ds(span_rows, arrived.shape[0])] = arrived[...]
    lanes = heads * block_len
    query_row = lax.broadcasted_iota(jnp.int32, (lanes, LANES), 0) % block_len
    lane = lax.broadcasted_iota(jnp.int32, (lanes, LANES), 1)
    causal = lane <= query_row
    pick_of_lane = lax.broadcasted_iota(jnp.int32, (1, LANES), 1) // block_len
    per_tile = LANES // block_len
    scale = latent_width ** (-0.5) * math.log2(math.e)

    def gather(turn):
        slot, inner = turn // per_shard, turn % per_shard
        local = jnp.bitwise_xor(me, groups[slot]) * per_shard + inner
        block = span * block_count + local
        if width > picks * block_len:
            rest = width - picks * block_len
            keys[turn, pl.ds(picks * block_len, rest)] = jnp.zeros((rest, latent_width), bf16)
        biases = []
        for pick in range(picks):
            target = chosen[local, pick]
            owner, within = split(target, block_count)
            near = near_slot(within, me, per_shard)
            source = jnp.where(owner == span, near, block_count + owner) * block_len
            keys[turn, pl.ds(pick * block_len, block_len)] = store[
                pl.ds(pl.multiple_of(source, block_len), block_len)
            ]
            biases.append(jnp.where((target < block) | (pick == 0), 0.0, -jnp.inf).astype(f32))
        query = absorbed[slot, :, pl.ds(inner * block_len, block_len), :].reshape(
            lanes, latent_width
        )
        scores = lax.dot_general(
            query, keys[turn], (((1,), (1,)), ((), ())), preferred_element_type=f32
        )
        return scores, biases

    def weigh(scores, biases):
        parts = []
        for tile in range(width // LANES):
            part = scores[:, tile * LANES : (tile + 1) * LANES]
            bias = jnp.full((1, LANES), -jnp.inf, f32)
            for inside in range(per_tile):
                pick = tile * per_tile + inside
                if pick < picks:
                    bias = jnp.where(pick_of_lane == inside, biases[pick], bias)
            part = part + bias
            if tile == 0:
                part = jnp.where(causal | (lane >= block_len), part, -jnp.inf)
            parts.append(part)
        top = parts[0]
        for part in parts[1:]:
            top = jnp.maximum(top, part)
        top = jnp.max(top, axis=1, keepdims=True)
        raised = [jnp.exp2((part - top) * scale) for part in parts]
        total = raised[0]
        for part in raised[1:]:
            total = total + part
        share = 1.0 / jnp.sum(total, axis=1, keepdims=True)
        return jnp.concatenate([(part * share).astype(bf16) for part in raised], axis=1)

    def mix(turn, weights):
        out = jnp.dot(weights, keys[turn], preferred_element_type=f32).astype(bf16)
        for head in range(heads):
            mixed[head, pl.ds(turn * block_len, block_len)] = out[
                head * block_len : (head + 1) * block_len
            ]

    turns = len(groups) * per_shard
    ahead = gather(0)
    for turn in range(turns):
        current = ahead
        if turn + 1 < turns:
            ahead = gather(turn + 1)
        mix(turn, weigh(*current))
    parts = []
    for head in range(heads):
        values = jnp.dot(mixed[head], value_absorb[head], preferred_element_type=f32)
        parts.append(rms(values, head_gain[pl.ds(head, 1)].astype(f32)).astype(bf16))
    head_out = jnp.concatenate(parts, axis=1)
    if len(outs) == len(groups):
        for slot, out in enumerate(outs):
            out[...] = head_out[slot * rows : (slot + 1) * rows]
    else:
        weight, own_heads, core_part = outs
        own_heads[...] = head_out[:rows]
        core_part[...] = jnp.dot(
            head_out[rows:], weight[...], preferred_element_type=f32
        ).astype(bf16)


def project_kernel(far, first, second, third, fourth, *rest):
    near, out = rest[:-1], rest[-1]
    span = lax.axis_index("kv")
    parity = jnp.bitwise_and(jnp.bitwise_xor(span, span >> 1), 1)
    depth = 2 * first.shape[0]
    direct = jnp.concatenate([first[...], second[...]], axis=0)
    relayed = jnp.concatenate([third[...], fourth[...]], axis=0)
    at = pl.multiple_of(parity * depth, depth)
    other = pl.multiple_of((1 - parity) * depth, depth)
    partial = jnp.dot(far[:, pl.ds(at, depth)], direct, preferred_element_type=f32)
    partial += jnp.dot(far[:, pl.ds(other, depth)], relayed, preferred_element_type=f32)
    if len(near) == 1:
        ready = near[0][...]
    else:
        heads_out, weight = near
        ready = jnp.dot(heads_out[...], weight[...], preferred_element_type=f32).astype(bf16)
    total = ready.astype(f32) + partial.astype(bf16).astype(f32)
    out[...] = total.astype(out.dtype)


def body(
    tokens,
    query_weight,
    latent_weight,
    key_absorb,
    query_gain,
    latent_gain,
    value_absorb,
    head_gain,
    out_weight,
    chosen,
):
    shards = lax.axis_size("tp")
    spans = lax.axis_size("kv")
    rows, model = tokens.shape
    heads, width, latent_width = key_absorb.shape
    block_count, picks = chosen.shape
    per_shard = block_count // shards
    block_len = rows // per_shard
    padded = -(-picks * block_len // LANES) * LANES
    shape = jax.ShapeDtypeStruct

    def swap(array, step):
        return lax.ppermute(array, "tp", [(i, i ^ step) for i in range(shards)])

    wanted = call(
        functools.partial(wanted_kernel, block_count), shape((spans, 1, LANES), jnp.int32), [VMEM]
    )(chosen)
    own = rms(
        jnp.dot(tokens, latent_weight, preferred_element_type=f32), latent_gain.astype(f32)
    ).astype(bf16)
    core = swap(own, 1)
    far = swap(own, 2)
    diag = swap(own, 3)
    asked = lax.all_to_all(wanted, "kv", split_axis=0, concat_axis=0, tiled=True)
    tokens_far = swap(tokens, 2)
    tokens_core = swap(tokens, 1)
    tokens_diag = swap(tokens_far, 1)
    parity = jnp.bitwise_and(lax.axis_index("kv") ^ (lax.axis_index("kv") >> 1), 1)
    quarter = out_weight.shape[0] // 4
    start = 2 * quarter * parity
    piece_a = lax.dynamic_slice(out_weight, (start, 0), (quarter, model))
    piece_b = lax.dynamic_slice(out_weight, (start + quarter, 0), (quarter, model))

    def relay(array, step):
        return lax.ppermute(array, "kv", [(i, i ^ step) for i in range(spans)])

    far_weights = [swap(piece_a, 2), swap(piece_b, 2)]
    far_weights.append(relay(far_weights[0], 1))
    far_weights.append(relay(far_weights[1], 2))
    outgoing = call(
        functools.partial(pick_kernel, per_shard),
        shape((spans * block_len, latent_width), bf16),
        [SMEM] + [VMEM] * 4,
        scratch=[pltpu.VMEM((block_count * block_len, latent_width), bf16)],
    )(asked, own, core, far, diag)
    arrived = lax.all_to_all(
        outgoing.reshape(spans, block_len, latent_width),
        "kv",
        split_axis=0,
        concat_axis=0,
        tiled=True,
    ).reshape(spans * block_len, latent_width)

    def absorb(pieces):
        return call(
            functools.partial(absorb_kernel, len(pieces)),
            [shape((len(pieces) // 2, heads, rows, latent_width), bf16)] * 2
            + [shape(chosen.shape, chosen.dtype), shape(head_gain.shape, bf16)],
            [VMEM] * (len(pieces) + 5),
            flops=2 * len(pieces) * rows * model * heads * width,
            grant=ABSORB,
        )(*pieces, query_weight, key_absorb, query_gain, chosen, head_gain)

    near_queries, far_queries, held, held_gain = absorb([tokens, tokens_core, tokens_far, tokens_diag])

    def attend(groups, queries, grant=None, weight=()):
        return call(
            functools.partial(attend_kernel, groups),
            [shape((rows, heads * width), bf16), shape((rows, model), bf16)]
            if weight
            else [shape((rows, heads * width), bf16)] * len(groups),
            [SMEM] + [VMEM] * (8 + len(weight)),
            scratch=[
                pltpu.VMEM(((block_count + spans) * block_len, latent_width), bf16),
                pltpu.VMEM((len(groups) * per_shard, padded, latent_width), bf16),
                pltpu.VMEM((heads, len(groups) * rows, latent_width), bf16),
            ],
            flops=8 * len(groups) * per_shard * heads * block_len * picks * block_len * latent_width,
            grant=grant,
        )(held, queries, own, core, far, diag, arrived, value_absorb, held_gain, *weight)

    far_own, far_core = attend((2, 3), far_queries, FAR)
    far_core = swap(far_core, 2)
    far_own = swap(far_own, 2)
    near_heads, near_part = attend((0, 1), near_queries, NEAR, (out_weight,))

    def project(far_heads, dtype, *near):
        return call(
            project_kernel,
            shape((rows, model), dtype),
            [VMEM] * (5 + len(near)),
            flops=2 * rows * heads * width * model,
        )(far_heads, *far_weights, *near)

    core_part = project(far_core, bf16, near_part)
    core_part = swap(core_part, 1)
    own_part = project(far_own, f32, near_heads, out_weight)
    return (own_part + core_part.astype(f32)).astype(bf16)


def solution(mesh):
    return jax.shard_map(
        body,
        mesh=mesh,
        in_specs=(
            P(("kv", "tp"), None),
            P(None, "tp"),
            P(),
            P("tp", None, None),
            P(),
            P(),
            P("tp", None, None),
            P("tp", None),
            P("tp", None),
            P("kv", None),
        ),
        out_specs=P(("kv", "tp"), None),
        check_vma=False,
    )
```
